32 devices in a mesh: sp: 16 (over z, y, core), tp: 2 (over x).
Axes of the slice: x: 2, y: 2, z: 4, core: 2. Of those that a mesh axis runs over, the one named last changes fastest.
Arguments:
- inputs: bfloat16 [4096, 4096], P('sp', 'tp'), may hold values from -20 to 20
- norm_gain: float32 [3, 4096], replicated, may hold values from 0.1 to 1.9
- in_weight: bfloat16 [3, 4096, 1024], P(None, 'tp', 'sp'), may hold values from -0.09375 to 0.09375
- pool_scale: float32 [3, 1024], replicated, may hold values from 0.1 to 1.9
- out_weight: bfloat16 [3, 1024, 4096], P(None, 'sp', 'tp'), may hold values from -0.1875 to 0.1875
Outputs:
- final_state: bfloat16 [4096, 4096], P('sp', 'tp')
The draws below stay inside these ranges and needn't reach their ends.
All inputs are finite; a program needn't handle non-finite values.
Results may differ from the reference program's by a relative error of at most 0.017.
Values may be sent and summed in bfloat16 or wider, within the bound.
A program may use at most 64 MiB of HBM per device.

```python
import jax
import jax.numpy as jnp
from jax import lax

D = 4096
P_SIZE = 1024
LAYERS = 3
TOKENS = 4096


def draw_inputs(key, part):
    column = lax.broadcasted_iota(jnp.float32, (1, D), 1) / D
    rough = jax.random.uniform(jax.random.fold_in(key, 2), (1, D), jnp.float32, 0.6, 1.4)
    column_scale = 0.35 * jnp.exp(jnp.log(10.0) * column) * rough
    base = jnp.clip(jax.random.normal(jax.random.fold_in(key, 1), (TOKENS, D), jnp.float32), -4.0, 4.0)
    return jnp.clip(base * column_scale, -20.0, 20.0).astype(jnp.bfloat16)


def levels(own_key, shape, split, least, largest):
    level = 1.0
    for dim, shards_of in split:
        heights = jax.random.uniform(jax.random.fold_in(jax.random.fold_in(own_key, 6), dim), (shards_of,), jnp.float32, least / len(split), largest / len(split))
        level = level * jnp.repeat(jnp.exp(heights), shape[dim] // shards_of).reshape((-1,) + (1,) * (len(shape) - 1 - dim))
    return level


def centred(own_key, extent, deviation, reach, pieces=(), dtype=jnp.bfloat16):
    values = jax.random.normal(own_key, extent, jnp.float32) * deviation
    if len(pieces) > 0:
        values = levels(own_key, extent, pieces, -0.22, 0.18) * values
    return jnp.clip(values, min=-reach, max=reach).astype(dtype)


def setup_inputs(seed: int = 0) -> dict:
    keys = jax.random.split(jax.random.key(seed), 6)
    inputs = draw_inputs(jax.random.fold_in(keys[5], 71), 0)
    norm_gain = jnp.clip(1.0 + 0.18 * jax.random.normal(keys[1], (LAYERS, D), jnp.float32), 0.1, 1.9)
    in_weight = centred(keys[2], (LAYERS, D, P_SIZE), D ** -0.5, 0.09375, ((1, 2), (2, 16)))
    pool_scale = jnp.clip(1.0 + 0.18 * jax.random.normal(keys[3], (LAYERS, P_SIZE), jnp.float32), 0.1, 1.9)
    out_weight = centred(keys[4], (LAYERS, P_SIZE, D), P_SIZE ** -0.5, 0.1875, ((1, 16), (2, 2)))
    return {"inputs": inputs, "norm_gain": norm_gain, "in_weight": in_weight, "pool_scale": pool_scale, "out_weight": out_weight}


epsilon = 1e-06
halo_rows = 16
group_count = 4

def window_means(extended, row_count, first_channel, first_pos, pool_total):
    width = extended.shape[1]
    channel = first_channel + lax.broadcasted_iota(jnp.int32, (1, width), 1)
    group_index = channel // (pool_total // group_count)
    window_len = jnp.left_shift(jnp.int32(2), group_index)
    running = jnp.zeros((row_count, width), jnp.float32)
    for offset in range(halo_rows):
        shifted = extended[halo_rows - offset:halo_rows - offset + row_count]
        running = running + jnp.where(offset < window_len, shifted, 0.0)
    position = first_pos + lax.broadcasted_iota(jnp.int32, (row_count, 1), 0)
    divisor = jnp.minimum(position + 1, window_len).astype(jnp.float32)
    return running / divisor - extended[halo_rows:]

def reference(inputs, norm_gain, in_weight, pool_scale, out_weight):
    current = inputs
    for layer_index in range(LAYERS):
        widened = current.astype(jnp.float32)
        inv_rms = lax.rsqrt(lax.optimization_barrier(jnp.mean(widened * widened, axis=1, keepdims=True)) + epsilon)
        normed = (widened * inv_rms * norm_gain[layer_index]).astype(jnp.bfloat16)
        pool_in = jnp.dot(normed, in_weight[layer_index], preferred_element_type=jnp.float32).astype(jnp.bfloat16)
        extended = jnp.concatenate([jnp.zeros((halo_rows, P_SIZE), jnp.float32), pool_in.astype(jnp.float32)], 0)
        means = window_means(extended, TOKENS, 0, 0, P_SIZE)
        mixed = (means * pool_scale[layer_index]).astype(jnp.bfloat16)
        branch = jnp.dot(mixed, out_weight[layer_index], preferred_element_type=jnp.float32)
        current = (widened + branch).astype(jnp.bfloat16)
    return current
```

```python
import functools

import jax
import jax.numpy as jnp
from jax import lax
from jax.experimental import pallas as pl
from jax.experimental.pallas import tpu as pltpu
from jax.sharding import PartitionSpec as P

EPS = 1e-06
REACH = 16
GROUPS = 4
MESH_ID = pl.DeviceIdType.MESH


def shift_sp(value):
    count = lax.axis_size("sp")
    return lax.ppermute(value, "sp", [(i, i + 1) for i in range(count - 1)])


def window_means(extended, row_count, first_channel, first_pos, pool_total):
    width = extended.shape[1]
    channel = first_channel + lax.broadcasted_iota(jnp.int32, (1, width), 1)
    window_len = jnp.left_shift(jnp.int32(2), channel // (pool_total // GROUPS))
    running = jnp.zeros((row_count, width), jnp.float32)
    for offset in range(REACH):
        shifted = extended[REACH - offset : REACH - offset + row_count]
        running = running + jnp.where(offset < window_len, shifted, 0.0)
    position = first_pos + lax.broadcasted_iota(jnp.int32, (row_count, 1), 0)
    divisor = jnp.minimum(position + 1, window_len).astype(jnp.float32)
    return running / divisor - extended[REACH:]


def plain_body(inputs, norm_gain, in_weight, pool_scale, out_weight):
    rows, feats = inputs.shape
    layers, features = norm_gain.shape
    pools = pool_scale.shape[1]
    part = pools // lax.axis_size("tp")
    t = lax.axis_index("tp")
    s = lax.axis_index("sp")
    current = inputs
    for layer in range(layers):
        in_all = lax.all_gather(in_weight[layer], "sp", axis=1, tiled=True)
        out_all = lax.all_gather(out_weight[layer], "sp", axis=0, tiled=True)
        wide = current.astype(jnp.float32)
        squares = lax.psum(jnp.sum(wide * wide, axis=1), "tp")
        inv_rms = lax.rsqrt(squares / features + EPS)[:, None]
        gain = lax.dynamic_slice_in_dim(norm_gain[layer], t * feats, feats)
        normed = (wide * inv_rms * gain).astype(jnp.bfloat16)
        partial = jnp.dot(normed, in_all, preferred_element_type=jnp.float32)
        pool_in = lax.psum_scatter(
            partial.astype(jnp.bfloat16), "tp", scatter_dimension=1, tiled=True
        )
        edge = shift_sp(pool_in[rows - REACH :])
        extended = jnp.concatenate([edge, pool_in], 0).astype(jnp.float32)
        means = window_means(extended, rows, t * part, s * rows, pools)
        scale = lax.dynamic_slice_in_dim(pool_scale[layer], t * part, part)
        mixed = (means * scale).astype(jnp.bfloat16)
        pooled = lax.all_gather(mixed, "tp", axis=1, tiled=True)
        branch = jnp.dot(pooled, out_all, preferred_element_type=jnp.float32)
        current = (current.astype(jnp.float32) + branch).astype(jnp.bfloat16)
    return current


def kernel(
    n_z, layers, halo,
    x_ref, gain_ref, wi_ref, scale_ref, wo_ref, o_ref,
    held, state, xg, edge, p_own, p_send, p_recv, mix, sq_send, sq_recv,
    w_send, w_recv, local_sem, a_send, a_recv,
):
    rows, feats = x_ref.shape
    total = rows + halo
    blocks = held.shape[1]
    half = mix.shape[3]
    pools = 2 * half
    phases = 2 * layers
    s = lax.axis_index("sp")
    t = lax.axis_index("tp")
    core = s % 2
    y = (s // 2) % 2
    z = s // 4

    def block_of(zz, yy, cc):
        return zz * 4 + yy * 2 + cc

    zs = [(z + d) % n_z for d in range(n_z)]
    y_mate = (block_of(z, 1 - y, core), t)
    c_mate = (block_of(z, y, 1 - core), t)
    x_mate = (s, 1 - t)
    after = ((s + 1) % blocks, t)
    before = ((s + blocks - 1) % blocks, t)
    z_mates = [(block_of(zz, y, core), t) for zz in zs[1:]]

    barrier = pltpu.get_barrier_semaphore()
    peers = z_mates + [y_mate, c_mate, x_mate, after, before]
    for peer in peers:
        pl.semaphore_signal(barrier, inc=1, device_id=peer, device_id_type=MESH_ID)
    pl.semaphore_wait(barrier, len(peers))

    sent = []

    def send(src, dst, send_sem, recv_sem, to):
        copy = pltpu.make_async_remote_copy(
            src_ref=src, dst_ref=dst, send_sem=send_sem, recv_sem=recv_sem,
            device_id=to, device_id_type=MESH_ID,
        )
        copy.start()
        sent.append(copy)

    def arrived(ref, sem):
        pltpu.make_async_remote_copy(
            src_ref=ref, dst_ref=ref, send_sem=sem, recv_sem=sem,
            device_id=c_mate, device_id_type=MESH_ID,
        ).wait_recv()

    def own(p):
        return (wi_ref if p % 2 == 0 else wo_ref).at[p // 2]

    count = [0] * phases

    def send_block(p, src, block, to):
        send(src, held.at[p, block], w_send.at[p, count[p]], w_recv.at[p, block], to)
        count[p] += 1

    def wait_block(p, block):
        arrived(held.at[p, block], w_recv.at[p, block])

    locals_ = []

    def issue_own(p):
        if p >= phases:
            return
        for mate in z_mates:
            send_block(p, own(p), s, mate)
        send_block(p, own(p), s, y_mate)
        send_block(p, own(p), s, c_mate)
        copy = pltpu.make_async_copy(own(p), held.at[p, s], local_sem.at[p])
        copy.start()
        locals_.append(copy)

    def pump_z(p):
        if p >= phases:
            return
        for zz in [zs[1], zs[-1]] + zs[2:-1]:
            block = block_of(zz, y, core)
            wait_block(p, block)
            send_block(p, held.at[p, block], block, y_mate)
            send_block(p, held.at[p, block], block, c_mate)

    def pump_y(p):
        for zz in [zs[0], zs[1], zs[-1]] + zs[2:-1]:
            block = block_of(zz, 1 - y, core)
            wait_block(p, block)
            send_block(p, held.at[p, block], block, c_mate)

    def finish(p):
        locals_[p].wait()
        for zz in zs:
            for yy in (y, 1 - y):
                wait_block(p, block_of(zz, yy, 1 - core))

    send(x_ref.at[pl.ds(rows - halo, halo)], edge, a_send.at[0], a_recv.at[0], after)
    issue_own(0)
    issue_own(1)

    @pl.loop(0, rows // REACH)
    def _(i):
        state[pl.ds(halo + i * REACH, REACH)] = x_ref[pl.ds(i * REACH, REACH)]

    arrived(edge, a_recv.at[0])
    keep = (s > 0).astype(jnp.float32)

    @pl.loop(0, halo // REACH)
    def _(i):
        part = edge[pl.ds(i * REACH, REACH)].astype(jnp.float32) * keep
        state[pl.ds(i * REACH, REACH)] = part.astype(jnp.bfloat16)

    def squares(layer):
        @pl.loop(0, total // REACH)
        def _(i):
            at = pl.ds(i * REACH, REACH)
            wide = state[at].astype(jnp.float32)
            value = jnp.sum(wide * wide, axis=1, keepdims=True)
            sq_send[layer, at] = jnp.broadcast_to(value, (REACH, 128))
            gain = gain_ref[pl.ds(layer, 1), pl.ds(pl.multiple_of(t * feats, 128), feats)]
            xg[at] = (wide * gain).astype(jnp.bfloat16)

        send(sq_send.at[layer], sq_recv.at[layer], a_send.at[1 + 3 * layer],
             a_recv.at[1 + 3 * layer], x_mate)

    def project(p, which):
        part = held[p, pl.ds(which * (blocks // 2), blocks // 2)].reshape(half, feats)
        return lax.dot_general(
            xg[...], part, (((1,), (1,)), ((), ())), preferred_element_type=jnp.float32
        )

    def compute_in(layer):
        p = 2 * layer
        sem = 2 + 3 * layer
        p_send[layer] = project(p, 1 - t).astype(jnp.bfloat16)
        send(p_send.at[layer], p_recv.at[layer], a_send.at[sem], a_recv.at[sem], x_mate)
        p_own[...] = project(p, t)
        arrived(sq_recv.at[layer], a_recv.at[sem - 1])
        arrived(p_recv.at[layer], a_recv.at[sem])
        lanes = 128
        row = lax.broadcasted_iota(jnp.int32, (total, lanes), 0)
        position = s * rows - halo + row
        mean = (sq_send[layer] + sq_recv[layer]) / (2 * feats)
        inv = lax.rsqrt(mean + EPS)
        for j in range(half // lanes):
            cols = pl.ds(j * lanes, lanes)
            joined = p_own[:, cols].astype(jnp.bfloat16).astype(jnp.float32)
            joined = joined + p_recv[layer, :, cols].astype(jnp.float32)
            base = (joined * inv).astype(jnp.bfloat16).astype(jnp.float32)
            channel = t * half + j * lanes + lax.broadcasted_iota(jnp.int32, (1, lanes), 1)
            group = channel // (pools // GROUPS)
            running = base
            width = 1
            picked = None
            for g in range(GROUPS):
                running = running + pltpu.roll(running, width, 0)
                width *= 2
                picked = running if picked is None else jnp.where(group >= g, running, picked)
            span = jnp.left_shift(jnp.int32(2), group)
            divisor = jnp.maximum(jnp.minimum(position + 1, span), 1).astype(jnp.float32)
            scale = scale_ref[
                pl.ds(layer, 1), pl.ds(pl.multiple_of(t * half + j * lanes, 128), lanes)
            ]
            mix[layer, t, :, cols] = ((picked / divisor - base) * scale).astype(jnp.bfloat16)
        send(mix.at[layer, t], mix.at[layer, t], a_send.at[sem + 1], a_recv.at[sem + 1], x_mate)

    def compute_out(layer):
        p = 2 * layer + 1
        sem = 3 + 3 * layer
        arrived(mix.at[layer, 1 - t], a_recv.at[sem])
        width = 256
        last = layer == layers - 1

        @pl.loop(0, feats // width)
        def _(n):
            cols = pl.ds(pl.multiple_of(n * width, width), width)
            low = held[p, pl.ds(0, blocks // 2), :, cols].reshape(half, width)
            high = held[p, pl.ds(blocks // 2, blocks // 2), :, cols].reshape(half, width)
            branch = jnp.dot(mix[layer, 0], low, preferred_element_type=jnp.float32)
            branch = branch + jnp.dot(mix[layer, 1], high, preferred_element_type=jnp.float32)
            new = (state[:, cols].astype(jnp.float32) + branch).astype(jnp.bfloat16)
            if last:
                o_ref[:, cols] = new[halo:]
            else:
                state[:, cols] = new

    squares(0)
    pump_z(0)
    for p in range(phases):
        issue_own(p + 2)
        pump_z(p + 1)
        pump_y(p)
        finish(p)
        if p % 2 == 0:
            compute_in(p // 2)
        else:
            compute_out(p // 2)
            if p // 2 + 1 < layers:
                squares(p // 2 + 1)
    for copy in sent:
        copy.wait_send()


def fused_body(inputs, norm_gain, in_weight, pool_scale, out_weight):
    rows, feats = inputs.shape
    layers = norm_gain.shape[0]
    half = pool_scale.shape[1] // 2
    blocks = lax.axis_size("sp")
    n_z = blocks // 4
    depth = out_weight.shape[1]
    halo = REACH * layers
    total = rows + halo
    bf, f32 = jnp.bfloat16, jnp.float32
    sends = 2 * (n_z - 1) + 3 + (n_z - 1) + n_z
    vmem = pl.BlockSpec(memory_space=pltpu.VMEM)
    return pl.pallas_call(
        functools.partial(kernel, n_z, layers, halo),
        out_shape=jax.ShapeDtypeStruct((rows, feats), bf),
        in_specs=[vmem] * 5,
        out_specs=vmem,
        scratch_shapes=[
            pltpu.VMEM((2 * layers, blocks, depth, feats), bf),
            pltpu.VMEM((total, feats), bf),
            pltpu.VMEM((total, feats), bf),
            pltpu.VMEM((halo, feats), bf),
            pltpu.VMEM((total, half), f32),
            pltpu.VMEM((layers, total, half), bf),
            pltpu.VMEM((layers, total, half), bf),
            pltpu.VMEM((layers, 2, total, half), bf),
            pltpu.VMEM((layers, total, 128), f32),
            pltpu.VMEM((layers, total, 128), f32),
            pltpu.SemaphoreType.DMA((2 * layers, sends)),
            pltpu.SemaphoreType.DMA((2 * layers, blocks)),
            pltpu.SemaphoreType.DMA((2 * layers,)),
            pltpu.SemaphoreType.DMA((1 + 3 * layers,)),
            pltpu.SemaphoreType.DMA((1 + 3 * layers,)),
        ],
        compiler_params=pltpu.CompilerParams(
            collective_id=0, has_side_effects=True, vmem_limit_bytes=60 * 1024 * 1024
        ),
    )(inputs, norm_gain, jnp.swapaxes(in_weight, 1, 2), pool_scale, out_weight)


def solution(mesh):
    n_sp, n_tp = mesh.shape["sp"], mesh.shape["tp"]
    fused = n_tp == 2 and n_sp == 16
    placed = (P("sp", "tp"), P(), P(None, "tp", "sp"), P(), P(None, "sp", "tp"))
    return jax.shard_map(
        fused_body if fused else plain_body,
        mesh=mesh, in_specs=placed, out_specs=P("sp", "tp"), check_vma=False,
    )
```

```python
import functools

import jax
import jax.numpy as jnp
from jax import lax
from jax.experimental import pallas as pl
from jax.experimental.pallas import tpu as pltpu
from jax.sharding import PartitionSpec as P

EPS = 1e-06
REACH = 16
GROUPS = 4
MESH_ID = pl.DeviceIdType.MESH


def shift_sp(value):
    count = lax.axis_size("sp")
    return lax.ppermute(value, "sp", [(i, i + 1) for i in range(count - 1)])


def window_means(extended, row_count, first_channel, first_pos, pool_total):
    width = extended.shape[1]
    channel = first_channel + lax.broadcasted_iota(jnp.int32, (1, width), 1)
    window_len = jnp.left_shift(jnp.int32(2), channel // (pool_total // GROUPS))
    running = jnp.zeros((row_count, width), jnp.float32)
    for offset in range(REACH):
        shifted = extended[REACH - offset : REACH - offset + row_count]
        running = running + jnp.where(offset < window_len, shifted, 0.0)
    position = first_pos + lax.broadcasted_iota(jnp.int32, (row_count, 1), 0)
    divisor = jnp.minimum(position + 1, window_len).astype(jnp.float32)
    return running / divisor - extended[REACH:]


def plain_body(inputs, norm_gain, in_weight, pool_scale, out_weight):
    rows, feats = inputs.shape
    layers, features = norm_gain.shape
    pools = pool_scale.shape[1]
    part = pools // lax.axis_size("tp")
    t = lax.axis_index("tp")
    s = lax.axis_index("sp")
    current = inputs
    for layer in range(layers):
        in_all = lax.all_gather(in_weight[layer], "sp", axis=1, tiled=True)
        out_all = lax.all_gather(out_weight[layer], "sp", axis=0, tiled=True)
        wide = current.astype(jnp.float32)
        squares = lax.psum(jnp.sum(wide * wide, axis=1), "tp")
        inv_rms = lax.rsqrt(squares / features + EPS)[:, None]
        gain = lax.dynamic_slice_in_dim(norm_gain[layer], t * feats, feats)
        normed = (wide * inv_rms * gain).astype(jnp.bfloat16)
        partial = jnp.dot(normed, in_all, preferred_element_type=jnp.float32)
        pool_in = lax.psum_scatter(
            partial.astype(jnp.bfloat16), "tp", scatter_dimension=1, tiled=True
        )
        edge = shift_sp(pool_in[rows - REACH :])
        extended = jnp.concatenate([edge, pool_in], 0).astype(jnp.float32)
        means = window_means(extended, rows, t * part, s * rows, pools)
        scale = lax.dynamic_slice_in_dim(pool_scale[layer], t * part, part)
        mixed = (means * scale).astype(jnp.bfloat16)
        pooled = lax.all_gather(mixed, "tp", axis=1, tiled=True)
        branch = jnp.dot(pooled, out_all, preferred_element_type=jnp.float32)
        current = (current.astype(jnp.float32) + branch).astype(jnp.bfloat16)
    return current


def kernel(
    n_z, layers, halo,
    x_ref, gain_ref, wi_ref, scale_ref, wo_ref, o_ref,
    held, state, xg, edge, p_own, p_send, p_recv, mix, sq_send, sq_recv,
    w_send, w_recv, local_sem, a_send, a_recv,
):
    rows, feats = x_ref.shape
    total = rows + halo
    blocks = held.shape[1]
    half = mix.shape[2] * mix.shape[4]
    pools = 2 * half
    phases = 2 * layers
    s = lax.axis_index("sp")
    t = lax.axis_index("tp")
    core = s % 2
    y = (s // 2) % 2
    z = s // 4

    def block_of(zz, yy, cc):
        return zz * 4 + yy * 2 + cc

    upper = z // 2
    near = z + 1 - 2 * (z % 2)
    across = n_z // 2 - upper
    far = (n_z - 1) * (1 - upper)
    at_end = jnp.logical_or(z == 0, z == n_z - 1)
    inside = jnp.logical_not(at_end)
    up, down = (z + 1) % n_z, (z + n_z - 1) % n_z
    has_up, has_down = z < n_z - 1, z > 0
    inner = jnp.where(upper == 0, up, down)
    outer = jnp.where(upper == 0, down, up)

    y_mate = (block_of(z, 1 - y, core), t)
    c_mate = (block_of(z, y, 1 - core), t)
    x_mate = (s, 1 - t)
    after = ((s + 1) % blocks, t)
    before = ((s + blocks - 1) % blocks, t)

    def along(zz):
        return (block_of(zz, y, core), t)

    barrier = pltpu.get_barrier_semaphore()
    peers = [along(up), along(down), y_mate, c_mate, x_mate, after, before]
    for peer in peers:
        pl.semaphore_signal(barrier, inc=1, device_id=peer, device_id_type=MESH_ID)
    pl.semaphore_wait(barrier, len(peers))

    sent = []

    def send(src, dst, send_sem, recv_sem, to, when=None):
        copy = pltpu.make_async_remote_copy(
            src_ref=src, dst_ref=dst, send_sem=send_sem, recv_sem=recv_sem,
            device_id=to, device_id_type=MESH_ID,
        )
        if when is None:
            copy.start()
        else:
            pl.when(when)(copy.start)
        sent.append((copy, when))

    def arrived(ref, sem):
        pltpu.make_async_remote_copy(
            src_ref=ref, dst_ref=ref, send_sem=sem, recv_sem=sem,
            device_id=c_mate, device_id_type=MESH_ID,
        ).wait_recv()

    depth = held.shape[2]
    whole, first, second = pl.ds(0, depth), pl.ds(0, depth // 2), pl.ds(depth // 2, depth // 2)

    def own(p):
        return (wi_ref if p % 2 == 0 else wo_ref).at[p // 2]

    count = [0] * phases

    def send_own(p, to, when=None):
        send(own(p), held.at[p, s], w_send.at[p, count[p]], w_recv.at[p, s, 0], to, when)
        count[p] += 1

    def forward(p, block, to, piece=None, when=None):
        piece = whole if piece is None else piece
        ref = held.at[p, block, piece]
        sem = w_recv.at[p, block, 1 if piece is second else 0]
        send(ref, ref, w_send.at[p, count[p]], sem, to, when)
        count[p] += 1

    def wait_block(p, block, piece=None):
        piece = whole if piece is None else piece
        arrived(held.at[p, block, piece], w_recv.at[p, block, 1 if piece is second else 0])

    locals_ = []

    def issue_own(p):
        if p >= phases:
            return
        send_own(p, along(up), has_up)
        send_own(p, along(down), has_down)
        send_own(p, y_mate)
        send_own(p, c_mate)
        copy = pltpu.make_async_copy(own(p), held.at[p, s], local_sem.at[p])
        copy.start()
        locals_.append(copy)

    def take_mate(p):
        block = block_of(z, 1 - y, core)
        wait_block(p, block)
        forward(p, block, along(inner), second, at_end)
        forward(p, block, c_mate)

    def take_near(p):
        block = block_of(near, y, core)
        wait_block(p, block)
        forward(p, block, along(inner), None, inside)
        forward(p, block, y_mate, first)
        forward(p, block, y_mate, second, at_end)
        forward(p, block, c_mate)

    def take_across(p):
        block = block_of(across, y, core)
        wait_block(p, block)
        forward(p, block, along(outer), None, inside)
        forward(p, block, y_mate)
        forward(p, block, c_mate)

    def take_far(p):
        block = block_of(far, y, core)
        wait_block(p, block)
        forward(p, block, along(outer), None, inside)
        forward(p, block, y_mate, first)
        forward(p, block, c_mate)

    def take_mate_near(p):
        block = block_of(near, 1 - y, core)
        wait_block(p, block, second)
        forward(p, block, along(inner), second, inside)
        wait_block(p, block, first)
        forward(p, block, c_mate)

    def take_mate_across(p):
        block = block_of(across, 1 - y, core)
        wait_block(p, block)
        forward(p, block, c_mate)

    def take_mate_far(p):
        block = block_of(far, 1 - y, core)
        wait_block(p, block, second)
        forward(p, block, along(outer), second, inside)
        wait_block(p, block, first)
        forward(p, block, c_mate)

    def finish(p):
        locals_[p].wait()
        for zz in range(n_z):
            for yy in range(2):
                wait_block(p, block_of(zz, yy, 1 - core))

    send(x_ref.at[pl.ds(rows - halo, halo)], edge, a_send.at[0], a_recv.at[0], after)
    issue_own(0)
    issue_own(1)

    @pl.loop(0, rows // REACH)
    def _(i):
        state[pl.ds(halo + i * REACH, REACH)] = x_ref[pl.ds(i * REACH, REACH)]

    arrived(edge, a_recv.at[0])
    keep = (s > 0).astype(jnp.float32)

    @pl.loop(0, halo // REACH)
    def _(i):
        part = edge[pl.ds(i * REACH, REACH)].astype(jnp.float32) * keep
        state[pl.ds(i * REACH, REACH)] = part.astype(jnp.bfloat16)

    def first_row(layer):
        return REACH * layer

    def from_row(start):
        return pl.ds(start, total - start)

    parts = mix.shape[2]
    slim = mix.shape[4]
    ahead = blocks // (2 * parts)

    def exchange(src, dst, sem):
        send(src, dst, a_send.at[sem], a_recv.at[sem], x_mate)

    def base_sem(layer):
        return 1 + (1 + 2 * parts) * layer

    def squares(layer):
        @pl.loop(first_row(layer) // REACH, total // REACH)
        def _(i):
            at = pl.ds(i * REACH, REACH)
            wide = state[at].astype(jnp.float32)
            value = jnp.sum(wide * wide, axis=1, keepdims=True)
            sq_send[layer, at] = jnp.broadcast_to(value, (REACH, 128))
            gain = gain_ref[pl.ds(layer, 1), pl.ds(pl.multiple_of(t * feats, 128), feats)]
            xg[at] = (wide * gain).astype(jnp.bfloat16)

        at = from_row(first_row(layer))
        exchange(sq_send.at[layer, at], sq_recv.at[layer, at], base_sem(layer))

    def project(layer, which, c):
        block = which * (blocks // 2) + c * ahead
        weight = held[2 * layer, pl.ds(block, ahead)].reshape(slim, feats)
        return lax.dot_general(
            xg[first_row(layer):], weight, (((1,), (1,)), ((), ())),
            preferred_element_type=jnp.float32,
        )

    def project_other(layer, c):
        at = from_row(first_row(layer))
        p_send[layer, c, at] = project(layer, 1 - t, c).astype(jnp.bfloat16)
        exchange(p_send.at[layer, c, at], p_recv.at[layer, c, at], base_sem(layer) + 1 + c)

    def project_own(layer, c):
        p_own[c, from_row(first_row(layer))] = project(layer, t, c)

    def pool(layer, c):
        sem = base_sem(layer)
        start = first_row(layer)
        at = from_row(start)
        if c == 0:
            arrived(sq_recv.at[layer, at], a_recv.at[sem])
        arrived(p_recv.at[layer, c, at], a_recv.at[sem + 1 + c])
        lanes = 128
        row = lax.broadcasted_iota(jnp.int32, (total - start, lanes), 0)
        position = s * rows - halo + start + row
        mean = (sq_send[layer, at] + sq_recv[layer, at]) / (2 * feats)
        inv = lax.rsqrt(mean + EPS)
        for j in range(slim // lanes):
            cols = pl.ds(j * lanes, lanes)
            joined = p_own[c, at, cols].astype(jnp.bfloat16).astype(jnp.float32)
            joined = joined + p_recv[layer, c, at, cols].astype(jnp.float32)
            base = (joined * inv).astype(jnp.bfloat16).astype(jnp.float32)
            lane = t * half + c * slim + j * lanes
            channel = lane + lax.broadcasted_iota(jnp.int32, (1, lanes), 1)
            group = channel // (pools // GROUPS)
            running = base
            width = 1
            picked = None
            for g in range(GROUPS):
                running = running + pltpu.roll(running, width, 0)
                width *= 2
                picked = running if picked is None else jnp.where(group >= g, running, picked)
            span = jnp.left_shift(jnp.int32(2), group)
            divisor = jnp.maximum(jnp.minimum(position + 1, span), 1).astype(jnp.float32)
            scale = scale_ref[pl.ds(layer, 1), pl.ds(pl.multiple_of(lane, 128), lanes)]
            mix[layer, t, c, at, cols] = ((picked / divisor - base) * scale).astype(jnp.bfloat16)
        at = from_row(first_row(layer + 1))
        exchange(mix.at[layer, t, c, at], mix.at[layer, t, c, at], sem + 1 + parts + c)

    def take_mix(layer):
        at = from_row(first_row(layer + 1))
        for c in range(parts):
            arrived(mix.at[layer, 1 - t, c, at], a_recv.at[base_sem(layer) + 1 + parts + c])

    def expand(layer, start, stop):
        p = 2 * layer + 1
        width = 256
        last = layer == layers - 1
        at = from_row(first_row(layer + 1))

        @pl.loop(start, stop)
        def _(n):
            cols = pl.ds(pl.multiple_of(n * width, width), width)
            mixed = jnp.concatenate(
                [mix[layer, h, c, at] for h in range(2) for c in range(parts)], axis=1
            )
            weight = held[p, :, :, cols].reshape(pools, width)
            branch = jnp.dot(mixed, weight, preferred_element_type=jnp.float32)
            new = (state[at, cols].astype(jnp.float32) + branch).astype(jnp.bfloat16)
            if last:
                o_ref[:, cols] = new
            else:
                state[at, cols] = new

    part = functools.partial

    def pieces(p):
        layer = p // 2
        if p % 2 == 0:
            todo = [part(project_other, layer, c) for c in range(parts)]
            todo += [part(project_own, layer, c) for c in range(parts)]
            return todo + [part(pool, layer, c) for c in range(parts)]
        columns = feats // 256
        step = columns // 4
        todo = [part(take_mix, layer)]
        todo += [part(expand, layer, k, k + step) for k in range(0, columns, step)]
        if layer + 1 < layers:
            todo.append(part(squares, layer + 1))
        return todo

    order_first = [take_mate, take_near, take_across, take_far]
    order_then = [take_mate_near, take_mate_across, take_mate_far, finish]
    waiting = []

    def work():
        if waiting:
            piece = waiting.pop(0)
            if piece is not None:
                piece()

    squares(0)
    for take in order_first:
        take(0)
    for p in range(phases):
        issue_own(p + 2)
        for take in order_first[:2]:
            if p + 1 < phases:
                take(p + 1)
                work()
        for take in order_then[:2]:
            take(p)
            work()
        for take in order_first[2:]:
            if p + 1 < phases:
                take(p + 1)
                work()
        for take in order_then[2:]:
            take(p)
            work()
        waiting.extend(pieces(p))
        work()
        if p % 2 == 0:
            work()
            work()
            work()
    while waiting:
        work()
    for copy, when in sent:
        if when is None:
            copy.wait_send()
        else:
            pl.when(when)(copy.wait_send)


def fused_body(inputs, norm_gain, in_weight, pool_scale, out_weight):
    rows, feats = inputs.shape
    layers = norm_gain.shape[0]
    half = pool_scale.shape[1] // 2
    blocks = lax.axis_size("sp")
    n_z = blocks // 4
    depth = out_weight.shape[1]
    halo = REACH * layers
    total = rows + halo
    bf, f32 = jnp.bfloat16, jnp.float32
    sends = 21
    parts = 2
    slim = half // parts
    vmem = pl.BlockSpec(memory_space=pltpu.VMEM)
    return pl.pallas_call(
        functools.partial(kernel, n_z, layers, halo),
        out_shape=jax.ShapeDtypeStruct((rows, feats), bf),
        in_specs=[vmem] * 5,
        out_specs=vmem,
        scratch_shapes=[
            pltpu.VMEM((2 * layers, blocks, depth, feats), bf),
            pltpu.VMEM((total, feats), bf),
            pltpu.VMEM((total, feats), bf),
            pltpu.VMEM((halo, feats), bf),
            pltpu.VMEM((parts, total, slim), f32),
            pltpu.VMEM((layers, parts, total, slim), bf),
            pltpu.VMEM((layers, parts, total, slim), bf),
            pltpu.VMEM((layers, 2, parts, total, slim), bf),
            pltpu.VMEM((layers, total, 128), f32),
            pltpu.VMEM((layers, total, 128), f32),
            pltpu.SemaphoreType.DMA((2 * layers, sends)),
            pltpu.SemaphoreType.DMA((2 * layers, blocks, 2)),
            pltpu.SemaphoreType.DMA((2 * layers,)),
            pltpu.SemaphoreType.DMA((1 + (1 + 2 * parts) * layers,)),
            pltpu.SemaphoreType.DMA((1 + (1 + 2 * parts) * layers,)),
        ],
        compiler_params=pltpu.CompilerParams(
            collective_id=0, has_side_effects=True, vmem_limit_bytes=60 * 1024 * 1024
        ),
    )(inputs, norm_gain, jnp.swapaxes(in_weight, 1, 2), pool_scale, out_weight)


def solution(mesh):
    n_sp, n_tp = mesh.shape["sp"], mesh.shape["tp"]
    fused = n_tp == 2 and n_sp == 16
    placed = (P("sp", "tp"), P(), P(None, "tp", "sp"), P(), P(None, "sp", "tp"))
    return jax.shard_map(
        fused_body if fused else plain_body,
        mesh=mesh, in_specs=placed, out_specs=P("sp", "tp"), check_vma=False,
    )
```
